32 devices in a mesh: fs: 8 (over z, x), tp: 4 (over y, core).
Axes of the slice: x: 2, y: 2, z: 4, core: 2. Of those that a mesh axis runs over, the one named last changes fastest.
Arguments:
- tokens: bfloat16 [4096, 2048], P(('fs', 'tp')), may hold values from -6 to 6
- norm_gain: float32 [2048], replicated, may hold values from 0.1 to 1.9
- up_weight: bfloat16 [2048, 8192], P('fs', 'tp'), may hold values from -0.125 to 0.125
- down_weight: bfloat16 [8192, 2048], P('tp', 'fs'), may hold values from -0.0625 to 0.0625
Outputs:
- mixed: bfloat16 [4096, 2048], P(('fs', 'tp'))
The draws below stay inside these ranges and needn't reach their ends.
All inputs are finite; a program needn't handle non-finite values.
Results may differ from the reference program's by a relative error of at most 0.013.
Values may be sent and summed in bfloat16 or wider, within the bound.
A program may use at most 64 MiB of HBM per device.

```python
import jax
import jax.numpy as jnp
from jax import lax

D = 2048
FF = 8192
TOKENS = 4096
N_TP = 4


def level_of(own_key, extent, shards, low, largest):
    loudness, own = 1.0, jax.random.fold_in(own_key, 6)
    for axis_at, parts in shards:
        heights = jnp.exp(jax.random.uniform(jax.random.fold_in(own, axis_at), (parts,), jnp.float32, low / len(shards), largest / len(shards)))
        loudness = loudness * jnp.repeat(heights, extent[axis_at] // parts).reshape([-1 if axis == axis_at else 1 for axis in range(len(extent))])
    return loudness


def normal_values(own_key, extent, deviation, reach, split=(), held_as=jnp.bfloat16):
    array = jax.random.normal(own_key, extent, jnp.float32) * deviation
    if len(split) > 0:
        array = level_of(own_key, extent, split, -0.22, 0.18) * array
    return jnp.clip(array, min=-reach, max=reach).astype(held_as)


def setup_inputs(seed: int = 0) -> dict:
    streams_of = jax.random.split(jax.random.key(seed), 5)
    return {
        "tokens": normal_values(streams_of[0], (TOKENS, D), 1.0, 6.0, ((0, 32),)),
        "norm_gain": jnp.clip(1.0 + 0.18 * jax.random.normal(streams_of[1], (D,), jnp.float32), 0.1, 1.9),
        "up_weight": normal_values(streams_of[2], (D, FF), D ** -0.5, 0.125, ((0, 8), (1, 4))),
        "down_weight": normal_values(streams_of[3], (FF, D), FF ** -0.5, 0.0625, ((0, 4), (1, 8))),
    }


epsilon = 1e-06

def reference(tokens, norm_gain, up_weight, down_weight):
    values = tokens.astype(jnp.float32)
    mean_square = lax.optimization_barrier(jnp.mean(values * values, axis=-1, keepdims=True))
    normed = (values * lax.rsqrt(mean_square + epsilon) * norm_gain).astype(jnp.bfloat16)
    preact = jnp.dot(normed, up_weight, preferred_element_type=jnp.float32)
    hidden = jnp.square(jnp.maximum(preact, 0.0)).astype(jnp.bfloat16)
    width = FF // N_TP
    total = jnp.zeros((tokens.shape[0], D), jnp.float32)
    for block in range(N_TP):
        columns = hidden[:, block * width:(block + 1) * width]
        rows_down = down_weight[block * width:(block + 1) * width, :]
        partial_value = jnp.dot(columns, rows_down, preferred_element_type=jnp.float32).astype(jnp.bfloat16)
        partial_value = lax.optimization_barrier(partial_value)
        total = total + partial_value.astype(jnp.float32)
    return total.astype(jnp.bfloat16)
```

```python
import functools
import math

import jax
import jax.numpy as jnp
from jax import lax
from jax.experimental import pallas as pl
from jax.experimental.pallas import tpu as pltpu
from jax.sharding import PartitionSpec as P

epsilon = 1e-06
MESH = pl.DeviceIdType.MESH
f32, bf16 = jnp.float32, jnp.bfloat16


def plain(tokens, norm_gain, up_weight, down_weight):
    values = tokens.astype(f32)
    mean_square = jnp.mean(values * values, axis=-1, keepdims=True)
    normed = (values * lax.rsqrt(mean_square + epsilon) * norm_gain).astype(bf16)
    up_whole = lax.all_gather(up_weight, "fs", axis=0, tiled=True)
    rows = lax.all_gather(normed, "tp", axis=0, tiled=True)
    preact = jnp.dot(rows, up_whole, preferred_element_type=f32)
    hidden = jnp.square(jnp.maximum(preact, 0.0)).astype(bf16)
    down_whole = lax.all_gather(down_weight, "fs", axis=1, tiled=True)
    partial_value = jnp.dot(hidden, down_whole, preferred_element_type=f32).astype(bf16)
    return lax.psum_scatter(partial_value, "tp", scatter_dimension=0, tiled=True)


def kernel(Z, X, Y, C, tok, gain, up, down, out,
           tokg, upg, downg, hid, part, cin, ysum, yin, zlo, zhi, zout, acc,
           wz_s, wz_r, wx_s, wx_r, tu_s, td_s, t_r, ty_s, ty_r, tc_s, tc_r,
           rc_s, rc_r, ry_s, ry_r, rz_s, rlo_r, rhi_r):
    T, D = tok.shape
    F = Z * X
    Dl = up.shape[0]
    B = upg.shape[1]
    fs, tp = lax.axis_index("fs"), lax.axis_index("tp")
    z, x = fs // X, fs % X
    y, c = tp // C, tp % C
    ox, oy, oc = X - 1 - x, Y - 1 - y, C - 1 - c

    def dev(zz=z, xx=x, yy=y, cc=c):
        return {"fs": zz * X + xx, "tp": yy * C + cc}

    def rcopy(src, dst, ss, rs, device):
        return pltpu.make_async_remote_copy(
            src_ref=src, dst_ref=dst, send_sem=ss, recv_sem=rs,
            device_id=device, device_id_type=MESH)

    barrier = pltpu.get_barrier_semaphore()
    peers = [dev(zz=(z + k) % Z) for k in range(1, Z)]
    peers += [dev(xx=ox), dev(yy=oy), dev(cc=oc)]
    for p in peers:
        pl.semaphore_signal(barrier, inc=1, device_id=p, device_id_type=MESH)

    def rows(yy, cc):
        return pl.ds(pl.multiple_of((cc * Y + yy) * T, T), T)

    mine = rows(y, c)

    RB = 32

    @pl.loop(0, T // RB)
    def _(i):
        r = pl.ds(pl.multiple_of(i * RB, RB), RB)
        v = tok[r, :].astype(f32)
        ms = jnp.mean(v * v, axis=-1, keepdims=True)
        w = pl.ds(pl.multiple_of((c * Y + y) * T + i * RB, RB), RB)
        tokg[z, w, :] = (v * lax.rsqrt(ms + epsilon) * gain[...]).astype(bf16)

    pl.semaphore_wait(barrier, len(peers))

    def tok_up(g):
        return rcopy(tokg.at[g, mine], tokg.at[g, mine], tu_s.at[g], t_r.at[g], dev(zz=z + 1))

    def tok_dn(g):
        return rcopy(tokg.at[g, mine], tokg.at[g, mine], td_s.at[g], t_r.at[g], dev(zz=z - 1))

    def tok_y(g):
        return rcopy(tokg.at[g, mine], tokg.at[g, mine], ty_s.at[g], ty_r.at[g], dev(yy=oy))

    def tok_c(g, k):
        w = rows(y if k == 0 else oy, c)
        return rcopy(tokg.at[g, w], tokg.at[g, w], tc_s.at[g, k], tc_r.at[g, k], dev(cc=oc))

    def tok_c_recv(g, k):
        w = rows(y if k == 0 else oy, oc)
        return rcopy(tokg.at[g, w], tokg.at[g, w], tc_s.at[g, k], tc_r.at[g, k], dev(cc=oc))

    def tok_y_recv(g):
        w = rows(oy, c)
        return rcopy(tokg.at[g, w], tokg.at[g, w], ty_s.at[g], ty_r.at[g], dev(yy=oy))

    def up_rows(f):
        return upg.at[pl.ds(pl.multiple_of(f * Dl, Dl), Dl)]

    def wz(zz, k):
        blk = pl.ds(pl.multiple_of(zz * B, B), B)
        if k == 0:
            return rcopy(up.at[:, blk], up_rows(fs), wz_s.at[0, zz], wz_r.at[0, z], dev(zz=zz))
        return rcopy(down.at[blk], downg.at[fs], wz_s.at[1, zz], wz_r.at[1, z], dev(zz=zz))

    def wz_recv(zz, k):
        dst = up_rows(zz * X + x) if k == 0 else downg.at[zz * X + x]
        return rcopy(dst, dst, wz_s.at[k, zz], wz_r.at[k, zz], dev(zz=zz))

    def wx(zz, k):
        dst = up_rows(zz * X + x) if k == 0 else downg.at[zz * X + x]
        return rcopy(dst, dst, wx_s.at[k, zz], wx_r.at[k, zz], dev(xx=ox))

    def wx_recv(zz, k):
        dst = up_rows(zz * X + ox) if k == 0 else downg.at[zz * X + ox]
        return rcopy(dst, dst, wx_s.at[k, zz], wx_r.at[k, zz], dev(xx=ox))

    def wx_own(k):
        blk = pl.ds(pl.multiple_of(z * B, B), B)
        src = up.at[:, blk] if k == 0 else down.at[blk]
        dst = up_rows(fs) if k == 0 else downg.at[fs]
        return rcopy(src, dst, wx_s.at[k, z], wx_r.at[k, z], dev(xx=ox))

    @pl.when(z < Z - 1)
    def _():
        tok_up(z).start()

    @pl.when(z > 0)
    def _():
        tok_dn(z).start()

    tok_y(z).start()
    tok_c(z, 0).start()
    wx_own(0).start()
    wx_own(1).start()
    for d in range(1, Z):
        for sgn in (-1, 1):
            zz = z + sgn * d

            @pl.when((zz >= 0) & (zz < Z))
            def _():
                wz(zz, 0).start()
                wz(zz, 1).start()

    own = pl.ds(pl.multiple_of(z * B, B), B)
    upg[pl.ds(pl.multiple_of(fs * Dl, Dl), Dl), :] = up[:, own]
    downg[fs] = down[own, :]

    def y_forward(g):
        tok_y_recv(g).wait_recv()
        tok_c(g, 1).start()

    for d in range(1, Z + 1):
        for sgn in (-1, 1):
            zz = z + sgn * d
            if d < Z:
                @pl.when((zz >= 0) & (zz < Z))
                def _():
                    tok_up(zz).wait_recv()
                    if sgn < 0:
                        @pl.when(z < Z - 1)
                        def _():
                            tok_up(zz).start()
                    else:
                        @pl.when(z > 0)
                        def _():
                            tok_dn(zz).start()
                    tok_y(zz).start()
                    tok_c(zz, 0).start()
                    for k in range(2):
                        wz_recv(zz, k).wait_recv()
                        wx(zz, k).start()
            if d == 1:
                if sgn > 0:
                    y_forward(z)
            else:
                back = z + sgn * (d - 1)

                @pl.when((back >= 0) & (back < Z))
                def _():
                    y_forward(back)

    for g in range(Z):
        for k in range(2):
            wx_recv(g, k).wait_recv()
            tok_c_recv(g, k).wait_recv()

    table = [sorted(range(Z), key=lambda g, a=a: -abs(g - a)) for a in range(Z)]

    def group(s):
        g = jnp.int32(table[0][s])
        for a in range(1, Z):
            g = jnp.where(z == a, jnp.int32(table[a][s]), g)
        return g

    NB = min(B, 256)

    def compute(g):
        @pl.loop(0, B // NB)
        def _(j):
            cols = pl.ds(pl.multiple_of(j * NB, NB), NB)
            h = jnp.maximum(jnp.dot(tokg[g], upg[:, cols], preferred_element_type=f32), 0.0)
            hid[:, cols] = (h * h).astype(bf16)

        @pl.loop(0, F)
        def _(f):
            cols = pl.ds(pl.multiple_of(f * Dl, Dl), Dl)
            v = jnp.dot(hid[...], downg[f], preferred_element_type=f32).astype(bf16)
            for cc in range(C):
                part[g, cc, :, cols] = v[cc * Y * T:(cc + 1) * Y * T]

    def sum_c(g):
        return rcopy(part.at[g, oc], cin.at[g], rc_s.at[g], rc_r.at[g], dev(cc=oc))

    def sum_y(g):
        return rcopy(ysum.at[g], yin.at[g], ry_s.at[g], ry_r.at[g], dev(yy=oy))

    def sum_up(g):
        return rcopy(zout.at[g], zlo.at[g], rz_s.at[g], rlo_r.at[g], dev(zz=z + 1))

    def sum_dn(g):
        return rcopy(zout.at[g], zhi.at[g], rz_s.at[g], rhi_r.at[g], dev(zz=z - 1))

    def step_y(g):
        sum_c(g).wait_recv()
        r = pl.ds(pl.multiple_of(oy * T, T), T)
        ysum[g] = (part[g, c, r, :].astype(f32) + cin[g, r, :].astype(f32)).astype(bf16)
        sum_y(g).start()

    for s in range(Z):
        g = group(s)
        compute(g)
        sum_c(g).start()
        if s > 0:
            step_y(group(s - 1))
    step_y(group(Z - 1))

    for s in range(Z):
        g = group(s)
        sum_y(g).wait_recv()
        r = pl.ds(pl.multiple_of(y * T, T), T)
        acc[...] = part[g, c, r, :].astype(f32) + cin[g, r, :].astype(f32) + yin[g].astype(f32)

        @pl.when((z <= g) & (z > 0))
        def _():
            sum_up(g).wait_recv()
            acc[...] += zlo[g].astype(f32)

        @pl.when((z >= g) & (z < Z - 1))
        def _():
            sum_dn(g).wait_recv()
            acc[...] += zhi[g].astype(f32)

        @pl.when(z == g)
        def _():
            out[...] = acc[...].astype(bf16)

        @pl.when(z < g)
        def _():
            zout[g] = acc[...].astype(bf16)
            sum_up(g).start()

        @pl.when(z > g)
        def _():
            zout[g] = acc[...].astype(bf16)
            sum_dn(g).start()

    for g in range(Z):
        @pl.when((z < Z - 1) & (g <= z))
        def _():
            tok_up(g).wait_send()

        @pl.when((z > 0) & (g >= z))
        def _():
            tok_dn(g).wait_send()

        tok_y(g).wait_send()
        for k in range(2):
            tok_c(g, k).wait_send()
            wx(g, k).wait_send()

        @pl.when(z != g)
        def _():
            wz(g, 0).wait_send()
            wz(g, 1).wait_send()
            sum_up(g).wait_send()

        sum_c(g).wait_send()
        sum_y(g).wait_send()


def solution(mesh):
    n_fs, n_tp = mesh.shape["fs"], mesh.shape["tp"]
    X = 2 ** (int(math.log2(n_fs)) // 2)
    Z = n_fs // X
    C = 2
    Y = n_tp // C
    placed = (P(("fs", "tp"), None), P(), P("fs", "tp"), P("tp", "fs"))

    def on_device(tokens, norm_gain, up_weight, down_weight):
        T, D = tokens.shape
        Dl, FFl = up_weight.shape
        B = FFl // Z
        if X != 2 or Y != 2 or Z * X != n_fs or Dl % 128 or B % 128 or T % 32:
            return plain(tokens, norm_gain, up_weight, down_weight)
        F = Z * X
        dma = pltpu.SemaphoreType.DMA
        vm = pl.BlockSpec(memory_space=pltpu.VMEM)
        return pl.pallas_call(
            functools.partial(kernel, Z, X, Y, C),
            out_shape=jax.ShapeDtypeStruct((T, D), bf16),
            in_specs=[vm] * 4,
            out_specs=vm,
            scratch_shapes=[
                pltpu.VMEM((Z, C * Y * T, D), bf16),
                pltpu.VMEM((D, B), bf16),
                pltpu.VMEM((F, B, Dl), bf16),
                pltpu.VMEM((C * Y * T, B), bf16),
                pltpu.VMEM((Z, C, Y * T, D), bf16),
                pltpu.VMEM((Z, Y * T, D), bf16),
                pltpu.VMEM((Z, T, D), bf16),
                pltpu.VMEM((Z, T, D), bf16),
                pltpu.VMEM((Z, T, D), bf16),
                pltpu.VMEM((Z, T, D), bf16),
                pltpu.VMEM((Z, T, D), bf16),
                pltpu.VMEM((T, D), f32),
                dma((2, Z)), dma((2, Z)), dma((2, Z)), dma((2, Z)),
                dma((Z,)), dma((Z,)), dma((Z,)), dma((Z,)), dma((Z,)),
                dma((Z, 2)), dma((Z, 2)),
                dma((Z,)), dma((Z,)), dma((Z,)), dma((Z,)),
                dma((Z,)), dma((Z,)), dma((Z,)),
            ],
            compiler_params=pltpu.CompilerParams(
                collective_id=0, has_side_effects=True, vmem_limit_bytes=60 * 2**20),
        )(tokens, norm_gain.reshape(1, D), up_weight, down_weight)

    return jax.shard_map(
        on_device, mesh=mesh, in_specs=placed, out_specs=P(("fs", "tp"), None), check_vma=False)
```

```python
import functools
import math

import jax
import jax.numpy as jnp
from jax import lax
from jax.experimental import pallas as pl
from jax.experimental.pallas import tpu as pltpu
from jax.sharding import PartitionSpec as P

epsilon = 1e-06
MESH = pl.DeviceIdType.MESH
f32, bf16 = jnp.float32, jnp.bfloat16


def plain(tokens, norm_gain, up_weight, down_weight):
    values = tokens.astype(f32)
    mean_square = jnp.mean(values * values, axis=-1, keepdims=True)
    normed = (values * lax.rsqrt(mean_square + epsilon) * norm_gain).astype(bf16)
    up_whole = lax.all_gather(up_weight, "fs", axis=0, tiled=True)
    rows = lax.all_gather(normed, "tp", axis=0, tiled=True)
    preact = jnp.dot(rows, up_whole, preferred_element_type=f32)
    hidden = jnp.square(jnp.maximum(preact, 0.0)).astype(bf16)
    down_whole = lax.all_gather(down_weight, "fs", axis=1, tiled=True)
    partial_value = jnp.dot(hidden, down_whole, preferred_element_type=f32).astype(bf16)
    return lax.psum_scatter(partial_value, "tp", scatter_dimension=0, tiled=True)


def kernel(Z, X, Y, C, tok, gain, up, down, out,
           tokg, upg, downg, hid, part, cin, zlo, zhi, zout, acc,
           wz_s, wz_r, wx_s, wx_r, wy_s, wy_r, wd_s, wd_r,
           tu_s, td_s, t_r, tc_s, tc_r, rc_s, rc_r, rz_s, rlo_r, rhi_r):
    T, D = tok.shape
    F = Z * X
    Dl = up.shape[0]
    B = upg.shape[2]
    fs, tp = lax.axis_index("fs"), lax.axis_index("tp")
    z, x = fs // X, fs % X
    y, c = tp // C, tp % C
    ox, oy, oc = X - 1 - x, Y - 1 - y, C - 1 - c

    def dev(zz=z, xx=x, yy=y, cc=c):
        return {"fs": zz * X + xx, "tp": yy * C + cc}

    def rcopy(src, dst, ss, rs, device):
        return pltpu.make_async_remote_copy(
            src_ref=src, dst_ref=dst, send_sem=ss, recv_sem=rs,
            device_id=device, device_id_type=MESH)

    barrier = pltpu.get_barrier_semaphore()
    peers = [dev(zz=(z + k) % Z) for k in range(1, Z)]
    peers += [dev(xx=ox), dev(yy=oy), dev(cc=oc)]
    for p in peers:
        pl.semaphore_signal(barrier, inc=1, device_id=p, device_id_type=MESH)

    def rows(cc):
        return pl.ds(pl.multiple_of(cc * T, T), T)

    mine = rows(c)

    RB = 32

    @pl.loop(0, T // RB)
    def _(i):
        r = pl.ds(pl.multiple_of(i * RB, RB), RB)
        v = tok[r, :].astype(f32)
        ms = jnp.mean(v * v, axis=-1, keepdims=True)
        w = pl.ds(pl.multiple_of(c * T + i * RB, RB), RB)
        tokg[z, w, :] = (v * lax.rsqrt(ms + epsilon) * gain[...]).astype(bf16)

    pl.semaphore_wait(barrier, len(peers))

    def tok_up(g):
        return rcopy(tokg.at[g, mine], tokg.at[g, mine], tu_s.at[g], t_r.at[g], dev(zz=z + 1))

    def tok_dn(g):
        return rcopy(tokg.at[g, mine], tokg.at[g, mine], td_s.at[g], t_r.at[g], dev(zz=z - 1))

    def tok_c(g, cc=c):
        w = rows(cc)
        return rcopy(tokg.at[g, w], tokg.at[g, w], tc_s.at[g], tc_r.at[g], dev(cc=oc))

    def piece(zz, xx, yy, k):
        f = zz * X + xx
        if k == 0:
            return upg.at[yy, pl.ds(pl.multiple_of(f * Dl, Dl), Dl)]
        return downg.at[yy, f]

    def own_piece(zz, k):
        blk = pl.ds(pl.multiple_of(zz * B, B), B)
        return up.at[:, blk] if k == 0 else down.at[blk]

    def wz(zz, k):
        return rcopy(own_piece(zz, k), piece(z, x, y, k), wz_s.at[k, zz], wz_r.at[k, z], dev(zz=zz))

    def wz_recv(zz, k):
        p = piece(zz, x, y, k)
        return rcopy(p, p, wz_s.at[k, zz], wz_r.at[k, zz], dev(zz=zz))

    def wx(zz, k, xx=x):
        p = piece(zz, xx, y, k)
        return rcopy(p, p, wx_s.at[k, zz], wx_r.at[k, zz], dev(xx=ox))

    def wy(zz, k, yy=y):
        p = piece(zz, x, yy, k)
        return rcopy(p, p, wy_s.at[k, zz], wy_r.at[k, zz], dev(yy=oy))

    def wd(zz, k):
        if k == 0:
            p = piece(zz, ox, y, 0)
            return rcopy(p, p, wd_s.at[k, zz], wd_r.at[k, zz], dev(yy=oy))
        p = piece(zz, x, oy, 1)
        return rcopy(p, p, wd_s.at[k, zz], wd_r.at[k, zz], dev(xx=ox))

    def wd_recv(zz, k):
        p = piece(zz, ox, oy, k)
        return rcopy(p, p, wd_s.at[k, zz], wd_r.at[k, zz], dev(yy=oy) if k == 0 else dev(xx=ox))

    def each(d, body):
        for sgn in (-1, 1):
            zz = z + sgn * d

            @pl.when((zz >= 0) & (zz < Z))
            def _():
                body(zz, sgn)

    def tokens_out():
        @pl.when(z < Z - 1)
        def _():
            tok_up(z).start()

        @pl.when(z > 0)
        def _():
            tok_dn(z).start()

        tok_c(z).start()

    def weights_out(zz, sgn):
        wz(zz, 0).start()
        wz(zz, 1).start()

    def tokens_on(zz, sgn):
        tok_up(zz).wait_recv()
        if sgn < 0:
            @pl.when(z < Z - 1)
            def _():
                tok_up(zz).start()
        else:
            @pl.when(z > 0)
            def _():
                tok_dn(zz).start()
        tok_c(zz).start()

    def weights_on(zz, sgn):
        for k in range(2):
            wz_recv(zz, k).wait_recv()
            wx(zz, k).start()
            wy(zz, k).start()

    def diagonal(zz, sgn=0):
        wx(zz, 0, ox).wait_recv()
        wd(zz, 0).start()
        wy(zz, 1, oy).wait_recv()
        wd(zz, 1).start()

    def send_own_plane():
        for k in range(2):
            src, dst = own_piece(z, k), piece(z, x, y, k)
            rcopy(src, dst, wx_s.at[k, z], wx_r.at[k, z], dev(xx=ox)).start()
            rcopy(src, dst, wy_s.at[k, z], wy_r.at[k, z], dev(yy=oy)).start()

    def keep_own():
        own = pl.ds(pl.multiple_of(z * B, B), B)
        upg[y, pl.ds(pl.multiple_of(fs * Dl, Dl), Dl), :] = up[:, own]
        downg[y, fs] = down[own, :]

    for d in range(1, Z):
        each(d, weights_out)
    tokens_out()
    send_own_plane()
    keep_own()
    diagonal(z)
    for d in range(1, Z):
        each(d, weights_on)
        if d > 1:
            each(d - 1, diagonal)
            each(d - 1, tokens_on)
    each(Z - 1, diagonal)
    each(Z - 1, tokens_on)

    for g in range(Z):
        for k in range(2):
            wx(g, 1, ox).wait_recv() if k else wy(g, 0, oy).wait_recv()
            wd_recv(g, k).wait_recv()
        tok_c(g, oc).wait_recv()

    table = [sorted(range(Z), key=lambda g, a=a: -abs(g - a)) for a in range(Z)]

    def group(s):
        g = jnp.int32(table[0][s])
        for a in range(1, Z):
            g = jnp.where(z == a, jnp.int32(table[a][s]), g)
        return g

    NB = min(B, 256)

    def compute(g):
        for yy in range(Y):
            @pl.loop(0, B // NB)
            def _(j):
                cols = pl.ds(pl.multiple_of(j * NB, NB), NB)
                h = jnp.maximum(jnp.dot(tokg[g], upg[yy, :, cols], preferred_element_type=f32), 0.0)
                hid[yy, :, cols] = (h * h).astype(bf16)

        @pl.loop(0, F)
        def _(f):
            cols = pl.ds(pl.multiple_of(f * Dl, Dl), Dl)
            v = jnp.dot(hid[0], downg[0, f], preferred_element_type=f32)
            for yy in range(1, Y):
                v = v + jnp.dot(hid[yy], downg[yy, f], preferred_element_type=f32)
            v = v.astype(bf16)
            for cc in range(C):
                part[g, cc, :, cols] = v[cc * T:(cc + 1) * T]

    def sum_c(g):
        return rcopy(part.at[g, oc], cin.at[g], rc_s.at[g], rc_r.at[g], dev(cc=oc))

    def sum_up(g):
        return rcopy(zout.at[g], zlo.at[g], rz_s.at[g], rlo_r.at[g], dev(zz=z + 1))

    def sum_dn(g):
        return rcopy(zout.at[g], zhi.at[g], rz_s.at[g], rhi_r.at[g], dev(zz=z - 1))

    def step_z(g):
        sum_c(g).wait_recv()
        acc[...] = part[g, c].astype(f32) + cin[g].astype(f32)

        @pl.when((z <= g) & (z > 0))
        def _():
            sum_up(g).wait_recv()
            acc[...] += zlo[g].astype(f32)

        @pl.when((z >= g) & (z < Z - 1))
        def _():
            sum_dn(g).wait_recv()
            acc[...] += zhi[g].astype(f32)

        @pl.when(z == g)
        def _():
            out[...] = acc[...].astype(bf16)

        @pl.when(z < g)
        def _():
            zout[g] = acc[...].astype(bf16)
            sum_up(g).start()

        @pl.when(z > g)
        def _():
            zout[g] = acc[...].astype(bf16)
            sum_dn(g).start()

    end = (z == 0) | (z == Z - 1)
    for s in range(Z):
        g = group(s)
        compute(g)
        sum_c(g).start()
        if s > 0:
            @pl.when(end)
            def _():
                step_z(group(s - 1))
    for s in range(Z):
        g = group(s)
        if s < Z - 1:
            @pl.when((z > 0) & (z < Z - 1))
            def _():
                step_z(g)
        else:
            step_z(g)

    for g in range(Z):
        @pl.when((z < Z - 1) & (g <= z))
        def _():
            tok_up(g).wait_send()

        @pl.when((z > 0) & (g >= z))
        def _():
            tok_dn(g).wait_send()

        tok_c(g).wait_send()
        for k in range(2):
            wx(g, k).wait_send()
            wy(g, k).wait_send()
            wd(g, k).wait_send()

        @pl.when(z != g)
        def _():
            wz(g, 0).wait_send()
            wz(g, 1).wait_send()
            sum_up(g).wait_send()

        sum_c(g).wait_send()


def solution(mesh):
    n_fs, n_tp = mesh.shape["fs"], mesh.shape["tp"]
    X = 2 ** (int(math.log2(n_fs)) // 2)
    Z = n_fs // X
    C = 2
    Y = n_tp // C
    placed = (P(("fs", "tp"), None), P(), P("fs", "tp"), P("tp", "fs"))

    def on_device(tokens, norm_gain, up_weight, down_weight):
        T, D = tokens.shape
        Dl, FFl = up_weight.shape
        B = FFl // Z
        if X != 2 or Y != 2 or Z * X != n_fs or Dl % 128 or B % 128 or T % 32:
            return plain(tokens, norm_gain, up_weight, down_weight)
        F = Z * X
        dma = pltpu.SemaphoreType.DMA
        vm = pl.BlockSpec(memory_space=pltpu.VMEM)
        return pl.pallas_call(
            functools.partial(kernel, Z, X, Y, C),
            out_shape=jax.ShapeDtypeStruct((T, D), bf16),
            in_specs=[vm] * 4,
            out_specs=vm,
            scratch_shapes=[
                pltpu.VMEM((Z, C * T, D), bf16),
                pltpu.VMEM((Y, D, B), bf16),
                pltpu.VMEM((Y, F, B, Dl), bf16),
                pltpu.VMEM((Y, C * T, B), bf16),
                pltpu.VMEM((Z, C, T, D), bf16),
                pltpu.VMEM((Z, T, D), bf16),
                pltpu.VMEM((Z, T, D), bf16),
                pltpu.VMEM((Z, T, D), bf16),
                pltpu.VMEM((Z, T, D), bf16),
                pltpu.VMEM((T, D), f32),
                *[dma((2, Z)) for _ in range(8)],
                *[dma((Z,)) for _ in range(10)],
            ],
            compiler_params=pltpu.CompilerParams(
                collective_id=0, has_side_effects=True, vmem_limit_bytes=60 * 2**20),
        )(tokens, norm_gain.reshape(1, D), up_weight, down_weight)

    return jax.shard_map(
        on_device, mesh=mesh, in_specs=placed, out_specs=P(("fs", "tp"), None), check_vma=False)
```

```python
import functools
import math

import jax
import jax.numpy as jnp
from jax import lax
from jax.experimental import pallas as pl
from jax.experimental.pallas import tpu as pltpu
from jax.sharding import PartitionSpec as P

epsilon = 1e-06
MESH = pl.DeviceIdType.MESH
H = 4
f32, bf16 = jnp.float32, jnp.bfloat16


def plain(tokens, norm_gain, up_weight, down_weight):
    values = tokens.astype(f32)
    mean_square = jnp.mean(values * values, axis=-1, keepdims=True)
    normed = (values * lax.rsqrt(mean_square + epsilon) * norm_gain).astype(bf16)
    up_whole = lax.all_gather(up_weight, "fs", axis=0, tiled=True)
    rows = lax.all_gather(normed, "tp", axis=0, tiled=True)
    preact = jnp.dot(rows, up_whole, preferred_element_type=f32)
    hidden = jnp.square(jnp.maximum(preact, 0.0)).astype(bf16)
    down_whole = lax.all_gather(down_weight, "fs", axis=1, tiled=True)
    partial_value = jnp.dot(hidden, down_whole, preferred_element_type=f32).astype(bf16)
    return lax.psum_scatter(partial_value, "tp", scatter_dimension=0, tiled=True)


def kernel(Z, X, Y, C, tok, gain, up, down, out,
           tokg, upg, downg, hid, part, cin, zlo, zhi, zout, acc,
           wz_s, wz_r, wx_s, wx_r, wy_s, wy_r, wd_s, wd_r,
           tu_s, td_s, t_r, tc_s, tc_r, rc_s, rc_r, rz_s, rlo_r, rhi_r):
    T, D = tok.shape
    F = Z * X
    Dl = up.shape[0]
    B = upg.shape[2]
    fs, tp = lax.axis_index("fs"), lax.axis_index("tp")
    z, x = fs // X, fs % X
    y, c = tp // C, tp % C
    ox, oy, oc = X - 1 - x, Y - 1 - y, C - 1 - c

    def dev(zz=z, xx=x, yy=y, cc=c):
        return {"fs": zz * X + xx, "tp": yy * C + cc}

    def rcopy(src, dst, ss, rs, device):
        return pltpu.make_async_remote_copy(
            src_ref=src, dst_ref=dst, send_sem=ss, recv_sem=rs,
            device_id=device, device_id_type=MESH)

    barrier = pltpu.get_barrier_semaphore()
    peers = [dev(zz=(z + k) % Z) for k in range(1, Z)]
    peers += [dev(xx=ox), dev(yy=oy), dev(cc=oc)]
    for p in peers:
        pl.semaphore_signal(barrier, inc=1, device_id=p, device_id_type=MESH)

    def rows(cc):
        return pl.ds(pl.multiple_of(cc * T, T), T)

    mine = rows(c)

    pl.semaphore_wait(barrier, len(peers))

    def tok_up(g):
        return rcopy(tokg.at[g, mine], tokg.at[g, mine], tu_s.at[g], t_r.at[g], dev(zz=z + 1))

    def tok_dn(g):
        return rcopy(tokg.at[g, mine], tokg.at[g, mine], td_s.at[g], t_r.at[g], dev(zz=z - 1))

    def tok_c(g, cc=c):
        w = rows(cc)
        return rcopy(tokg.at[g, w], tokg.at[g, w], tc_s.at[g], tc_r.at[g], dev(cc=oc))

    def piece(zz, xx, yy, k):
        f = zz * X + xx
        if k == 0:
            return upg.at[yy, pl.ds(pl.multiple_of(f * Dl, Dl), Dl)]
        return downg.at[yy, f]

    def own_piece(zz, k):
        blk = pl.ds(pl.multiple_of(zz * B, B), B)
        return up.at[:, blk] if k == 0 else down.at[blk]

    def wz(zz, k):
        return rcopy(own_piece(zz, k), piece(z, x, y, k), wz_s.at[k, zz], wz_r.at[k, z], dev(zz=zz))

    def wz_recv(zz, k):
        p = piece(zz, x, y, k)
        return rcopy(p, p, wz_s.at[k, zz], wz_r.at[k, zz], dev(zz=zz))

    def wx(zz, k, xx=x):
        p = piece(zz, xx, y, k)
        return rcopy(p, p, wx_s.at[k, zz], wx_r.at[k, zz], dev(xx=ox))

    def wy(zz, k, yy=y):
        p = piece(zz, x, yy, k)
        return rcopy(p, p, wy_s.at[k, zz], wy_r.at[k, zz], dev(yy=oy))

    def wd(zz, k):
        if k == 0:
            p = piece(zz, ox, y, 0)
            return rcopy(p, p, wd_s.at[k, zz], wd_r.at[k, zz], dev(yy=oy))
        p = piece(zz, x, oy, 1)
        return rcopy(p, p, wd_s.at[k, zz], wd_r.at[k, zz], dev(xx=ox))

    def wd_recv(zz, k):
        p = piece(zz, ox, oy, k)
        return rcopy(p, p, wd_s.at[k, zz], wd_r.at[k, zz], dev(yy=oy) if k == 0 else dev(xx=ox))

    def each(d, body):
        for sgn in (-1, 1):
            zz = z + sgn * d

            @pl.when((zz >= 0) & (zz < Z))
            def _():
                body(zz, sgn)

    def tokens_out():
        @pl.when(z < Z - 1)
        def _():
            tok_up(z).start()

        @pl.when(z > 0)
        def _():
            tok_dn(z).start()

        tok_c(z).start()

    def weights_out(zz, sgn):
        wz(zz, 0).start()
        wz(zz, 1).start()

    def tokens_on(zz, sgn):
        tok_up(zz).wait_recv()
        if sgn < 0:
            @pl.when(z < Z - 1)
            def _():
                tok_up(zz).start()
        else:
            @pl.when(z > 0)
            def _():
                tok_dn(zz).start()
        tok_c(zz).start()

    def weights_on(zz, sgn):
        for k in range(2):
            wz_recv(zz, k).wait_recv()
            wx(zz, k).start()
            wy(zz, k).start()

    def diagonal(zz, sgn=0):
        wx(zz, 0, ox).wait_recv()
        wd(zz, 0).start()
        wy(zz, 1, oy).wait_recv()
        wd(zz, 1).start()

    def send_own_plane():
        for k in range(2):
            src, dst = own_piece(z, k), piece(z, x, y, k)
            rcopy(src, dst, wx_s.at[k, z], wx_r.at[k, z], dev(xx=ox)).start()
            rcopy(src, dst, wy_s.at[k, z], wy_r.at[k, z], dev(yy=oy)).start()

    def keep_own():
        own = pl.ds(pl.multiple_of(z * B, B), B)
        upg[y, pl.ds(pl.multiple_of(fs * Dl, Dl), Dl), :] = up[:, own]
        downg[y, fs] = down[own, :]

    for d in range(1, Z):
        each(d, weights_out)
    send_own_plane()
    RB = 32

    @pl.loop(0, T // RB)
    def _(i):
        r = pl.ds(pl.multiple_of(i * RB, RB), RB)
        v = tok[r, :].astype(f32)
        ms = jnp.mean(v * v, axis=-1, keepdims=True)
        w = pl.ds(pl.multiple_of(c * T + i * RB, RB), RB)
        tokg[z, w, :] = (v * lax.rsqrt(ms + epsilon) * gain[...]).astype(bf16)

    tokens_out()
    keep_own()
    diagonal(z)
    order = list(range(1, Z))
    for i, d in enumerate(order):
        each(d, weights_on)
        if i > 0:
            each(order[i - 1], diagonal)
            each(i, tokens_on)
    each(order[-1], diagonal)
    each(Z - 1, tokens_on)

    for g in range(Z):
        for k in range(2):
            wx(g, 1, ox).wait_recv() if k else wy(g, 0, oy).wait_recv()
            wd_recv(g, k).wait_recv()
        tok_c(g, oc).wait_recv()

    table = [sorted(range(Z), key=lambda g, a=a: -abs(g - a)) for a in range(Z)]

    def group(s):
        g = jnp.int32(table[0][s])
        for a in range(1, Z):
            g = jnp.where(z == a, jnp.int32(table[a][s]), g)
        return g

    NB = min(B, 256)

    def compute(g):
        for yy in range(Y):
            @pl.loop(0, B // NB)
            def _(j):
                cols = pl.ds(pl.multiple_of(j * NB, NB), NB)
                h = jnp.maximum(jnp.dot(tokg[g], upg[yy, :, cols], preferred_element_type=f32), 0.0)
                hid[yy, :, cols] = (h * h).astype(bf16)

    def project(g, h):
        @pl.loop(h * (F // H), (h + 1) * (F // H))
        def _(f):
            cols = pl.ds(pl.multiple_of(f * Dl, Dl), Dl)
            v = jnp.dot(hid[0], downg[0, f], preferred_element_type=f32)
            for yy in range(1, Y):
                v = v + jnp.dot(hid[yy], downg[yy, f], preferred_element_type=f32)
            v = v.astype(bf16)
            for cc in range(C):
                part[g, cc, :, cols] = v[cc * T:(cc + 1) * T]

    def cut(h):
        return pl.ds(h * (D // H), D // H)

    def sum_c(g, h):
        return rcopy(part.at[g, oc, :, cut(h)], cin.at[g, :, cut(h)], rc_s.at[h, g], rc_r.at[h, g], dev(cc=oc))

    def sum_up(g, h):
        return rcopy(zout.at[g, :, cut(h)], zlo.at[g, :, cut(h)], rz_s.at[h, g], rlo_r.at[h, g], dev(zz=z + 1))

    def sum_dn(g, h):
        return rcopy(zout.at[g, :, cut(h)], zhi.at[g, :, cut(h)], rz_s.at[h, g], rhi_r.at[h, g], dev(zz=z - 1))

    def step_z(g, h):
        w = cut(h)
        sum_c(g, h).wait_recv()
        acc[:, w] = part[g, c, :, w].astype(f32) + cin[g, :, w].astype(f32)

        @pl.when((z <= g) & (z > 0))
        def _():
            sum_up(g, h).wait_recv()
            acc[:, w] += zlo[g, :, w].astype(f32)

        @pl.when((z >= g) & (z < Z - 1))
        def _():
            sum_dn(g, h).wait_recv()
            acc[:, w] += zhi[g, :, w].astype(f32)

        @pl.when(z == g)
        def _():
            out[:, w] = acc[:, w].astype(bf16)

        @pl.when(z < g)
        def _():
            zout[g, :, w] = acc[:, w].astype(bf16)
            sum_up(g, h).start()

        @pl.when(z > g)
        def _():
            zout[g, :, w] = acc[:, w].astype(bf16)
            sum_dn(g, h).start()

    end = (z == 0) | (z == Z - 1)
    items = [(s, h) for s in range(Z) for h in range(H)]
    for i, (s, h) in enumerate(items):
        g = group(s)
        if h == 0:
            compute(g)
        project(g, h)
        sum_c(g, h).start()
        if i > 0 and items[i - 1][0] < Z - 1:
            @pl.when(end)
            def _():
                step_z(group(items[i - 1][0]), items[i - 1][1])
    for s, h in items:
        if s < Z - 1:
            @pl.when((z > 0) & (z < Z - 1))
            def _():
                step_z(group(s), h)
        else:
            step_z(group(s), h)

    for g in range(Z):
        @pl.when((z < Z - 1) & (g <= z))
        def _():
            tok_up(g).wait_send()

        @pl.when((z > 0) & (g >= z))
        def _():
            tok_dn(g).wait_send()

        tok_c(g).wait_send()
        for k in range(2):
            wx(g, k).wait_send()
            wy(g, k).wait_send()
            wd(g, k).wait_send()

        @pl.when(z != g)
        def _():
            wz(g, 0).wait_send()
            wz(g, 1).wait_send()
            for h in range(H):
                sum_up(g, h).wait_send()

        for h in range(H):
            sum_c(g, h).wait_send()


def solution(mesh):
    n_fs, n_tp = mesh.shape["fs"], mesh.shape["tp"]
    X = 2 ** (int(math.log2(n_fs)) // 2)
    Z = n_fs // X
    C = 2
    Y = n_tp // C
    placed = (P(("fs", "tp"), None), P(), P("fs", "tp"), P("tp", "fs"))

    def on_device(tokens, norm_gain, up_weight, down_weight):
        T, D = tokens.shape
        Dl, FFl = up_weight.shape
        B = FFl // Z
        if X != 2 or Y != 2 or Z * X != n_fs or Dl % 128 or B % 128 or T % 32 or D % (128 * H):
            return plain(tokens, norm_gain, up_weight, down_weight)
        F = Z * X
        dma = pltpu.SemaphoreType.DMA
        vm = pl.BlockSpec(memory_space=pltpu.VMEM)
        return pl.pallas_call(
            functools.partial(kernel, Z, X, Y, C),
            out_shape=jax.ShapeDtypeStruct((T, D), bf16),
            in_specs=[vm] * 4,
            out_specs=vm,
            scratch_shapes=[
                pltpu.VMEM((Z, C * T, D), bf16),
                pltpu.VMEM((Y, D, B), bf16),
                pltpu.VMEM((Y, F, B, Dl), bf16),
                pltpu.VMEM((Y, C * T, B), bf16),
                pltpu.VMEM((Z, C, T, D), bf16),
                pltpu.VMEM((Z, T, D), bf16),
                pltpu.VMEM((Z, T, D), bf16),
                pltpu.VMEM((Z, T, D), bf16),
                pltpu.VMEM((Z, T, D), bf16),
                pltpu.VMEM((T, D), f32),
                *[dma((2, Z)) for _ in range(8)],
                *[dma((Z,)) for _ in range(5)],
                *[dma((H, Z)) for _ in range(5)],
            ],
            compiler_params=pltpu.CompilerParams(
                collective_id=0, has_side_effects=True, vmem_limit_bytes=60 * 2**20),
        )(tokens, norm_gain.reshape(1, D), up_weight, down_weight)

    return jax.shard_map(
        on_device, mesh=mesh, in_specs=placed, out_specs=P(("fs", "tp"), None), check_vma=False)
```
